32 devices in a mesh: ep: 8 (over z, x), tp: 4 (over y, core).
Axes of the slice: x: 2, y: 2, z: 4, core: 2. Of those that a mesh axis runs over, the one named last changes fastest.
Arguments:
- hidden_in: bfloat16 [256, 4096], P('ep'), may hold values from -6 to 6
- norm_gain: float32 [4096], replicated, may hold values from 0.1 to 1.9
- group_ids: int32 [256], P('ep'), may hold values from 0 to 1, as said below
- inner_ids: int32 [256, 4], P('ep'), may hold values from 0 to 7, as said below
- group_prob: float32 [256], P('ep'), may hold values from 0.25 to 1
- expert_prob: float32 [256, 4], P('ep'), may hold values from 0.1 to 1
- w_gate: bfloat16 [16, 4096, 1024], P('ep', None, 'tp'), may hold values from -0.09375 to 0.09375
- w_up: bfloat16 [16, 4096, 1024], P('ep', None, 'tp'), may hold values from -0.09375 to 0.09375
- w_down: bfloat16 [16, 1024, 4096], P('ep', None, 'tp'), may hold values from -0.1875 to 0.1875
Outputs:
- moe_out: bfloat16 [256, 4096], P('ep', 'tp')
The draws below stay inside these ranges and needn't reach their ends.
Inputs may be any that keep to these rules, and one draw needn't show every extreme that they name: `group_ids`: among the 32 tokens of one index of ep no group is named by more than 16 tokens; one group is named by exactly 16 of them, and all of these name one common expert of it. `inner_ids`: each row names 4 different experts of the token's group.
All inputs are finite; a program needn't handle non-finite values.
Results may differ from the reference program's by a relative error of at most 0.0069.
Values may be sent and summed in bfloat16 or wider, within the bound.
No kernel may reach another device: no remote copies, remote signals or barrier semaphores. Data moves between devices by JAX's collectives and lax.ppermute only.
A program may use at most 64 MiB of HBM per device.

```python
import jax
import jax.numpy as jnp
from jax import lax

D = 4096
DE = 1024
EPG = 8
TOP = 4
TOK_DEV = 32
CAP = 16
EXPERTS = 16
GROUPS = 2
TOKENS = 256


def routing(key):
    subkeys = jax.random.split(jax.random.fold_in(key, 7), 8)
    block_count = TOKENS // TOK_DEV
    group_order = jax.random.permutation(subkeys[0], GROUPS)
    chosen = jnp.minimum(jax.random.randint(subkeys[1], (block_count,), 0, GROUPS), jax.random.randint(subkeys[2], (block_count,), 0, GROUPS))
    hot_group = group_order[chosen]
    others = jax.random.randint(subkeys[3], (block_count, TOK_DEV), 0, GROUPS - 1)
    others = jnp.where(others >= hot_group[:, None], others + 1, others)
    places = jax.vmap(lambda single: jax.random.permutation(single, TOK_DEV))(jax.random.split(subkeys[4], block_count))
    forced = places < CAP
    groups = jnp.where(forced, hot_group[:, None], others)
    inner = jax.vmap(lambda single: jax.random.permutation(single, EPG))(jax.random.split(subkeys[5], TOKENS))[:, :TOP]
    inner = inner.reshape(block_count, TOK_DEV, TOP)
    common = jax.random.randint(subkeys[6], (block_count,), 0, EPG)
    contains = jnp.any(inner == common[:, None, None], axis=-1)
    first = jnp.where(forced & jnp.logical_not(contains), common[:, None], inner[:, :, 0])
    inner = inner.at[:, :, 0].set(first)
    return (groups.reshape(TOKENS).astype(jnp.int32), inner.reshape(TOKENS, TOP).astype(jnp.int32))


def draw_group_ids(key, part):
    return routing(key)[0]


def draw_inner_ids(key, part):
    return routing(key)[1]


def block_scale(rng, extent, pieces, smallest, largest):
    level = 1.0
    for dim, shards_of in pieces:
        draws = jax.random.uniform(jax.random.fold_in(jax.random.fold_in(rng, 6), dim), (shards_of,), jnp.float32, smallest / len(pieces), largest / len(pieces))
        level = level * jnp.repeat(jnp.exp(draws), extent[dim] // shards_of).reshape((-1,) + (1,) * (len(extent) - 1 - dim))
    return level


def gaussian(key, extent, width, reach, cuts=(), kind=jnp.bfloat16):
    entries = width * jax.random.normal(key, extent, jnp.float32)
    if cuts:
        entries = entries * block_scale(key, extent, cuts, -0.22, 0.18)
    return jnp.clip(entries, -reach, reach).astype(kind)


def setup_inputs(seed: int = 0) -> dict:
    keys = jax.random.split(jax.random.key(seed), 10)
    hidden_in = gaussian(keys[0], (TOKENS, D), 1.0, 6.0, ((0, 8),))
    norm_gain = jnp.clip(1.0 + 0.18 * jax.random.normal(keys[1], (D,), jnp.float32), 0.1, 1.9)
    group_ids = draw_group_ids(jax.random.fold_in(keys[9], 71), 0)
    inner_ids = draw_inner_ids(jax.random.fold_in(keys[9], 71), 0)
    group_prob = jnp.clip(0.25 + 0.75 * jax.random.uniform(keys[4], (TOKENS,), jnp.float32) ** block_scale(keys[4], (TOKENS,), ((0, 8),), -0.2, 0.2), 0.25, 1.0)
    expert_prob = jnp.clip(0.1 + 0.9 * jax.random.uniform(keys[5], (TOKENS, TOP), jnp.float32) ** block_scale(keys[5], (TOKENS, TOP), ((0, 8),), -0.2, 0.2), 0.1, 1.0)
    w_gate = gaussian(keys[6], (EXPERTS, D, DE), D ** -0.5, 0.09375, ((0, 8), (2, 4)))
    w_up = gaussian(keys[7], (EXPERTS, D, DE), D ** -0.5, 0.09375, ((0, 8), (2, 4)))
    w_down = gaussian(keys[8], (EXPERTS, DE, D), DE ** -0.5, 0.1875, ((0, 8), (2, 4)))
    return {"hidden_in": hidden_in, "norm_gain": norm_gain, "group_ids": group_ids, "inner_ids": inner_ids, "group_prob": group_prob, "expert_prob": expert_prob, "w_gate": w_gate, "w_up": w_up, "w_down": w_down}


EPS = 1e-06

def reference(hidden_in, norm_gain, group_ids, inner_ids, group_prob, expert_prob, w_gate, w_up, w_down):
    widened = hidden_in.astype(jnp.float32)
    normed = (widened * lax.rsqrt(lax.optimization_barrier(jnp.mean(widened * widened, axis=-1, keepdims=True)) + EPS) * norm_gain).astype(jnp.bfloat16)
    expert_ids = group_ids[:, None] * EPG + inner_ids
    scaled = group_prob[:, None] * expert_prob
    route = lax.optimization_barrier(jnp.sum(jax.nn.one_hot(expert_ids, EXPERTS, dtype=jnp.float32) * scaled[:, :, None], axis=1))

    def one_expert(combined, inputs):
        gate_w, up_w, down_w, column = inputs
        gate_proj = jnp.dot(normed, gate_w, preferred_element_type=jnp.float32)
        up_proj = jnp.dot(normed, up_w, preferred_element_type=jnp.float32)
        activation = (jax.nn.silu(gate_proj) * up_proj * column[:, None]).astype(jnp.bfloat16)
        return (combined + jnp.dot(activation, down_w, preferred_element_type=jnp.float32), None)
    start = jnp.zeros((TOKENS, D), jnp.float32)
    combined, _ = lax.scan(one_expert, start, (w_gate, w_up, w_down, route.T))
    return combined.astype(jnp.bfloat16)
```

```python
import jax
import jax.numpy as jnp
from jax import lax
from jax.experimental import pallas as pl
from jax.experimental.pallas import tpu as pltpu
from jax.sharding import PartitionSpec as P

EPG = 8
EPS = 1e-06
LANES = 128
ANY = pl.BlockSpec(memory_space=pl.ANY)
BF16 = jnp.bfloat16
F32 = jnp.float32


def split3(value):
    high = value.astype(BF16)
    rest = value - high.astype(F32)
    mid = rest.astype(BF16)
    low = (rest - mid.astype(F32)).astype(BF16)
    return high, mid, low


def half_copies(sources, target, sems, which):
    half = target.shape[2]
    start = pl.multiple_of(which * half, LANES)
    return [
        pltpu.make_async_copy(
            source.at[e, pl.ds(start, half), :], target.at[e, m], sems.at[e, m]
        )
        for e in range(target.shape[0])
        for m, source in enumerate(sources)
    ]


def dispatch_kernel(*refs):
    sources, weights, (send, slots, first), targets = refs[:6], refs[6:8], refs[8:11], refs[11:17]
    sems, weight_sems = refs[17:]
    core = lax.axis_index("tp") % 2
    copies = [
        pltpu.make_async_copy(source, target, sems.at[n])
        for n, (source, target) in enumerate(zip(sources, targets))
    ]
    weight_copies = half_copies(weights, first, weight_sems, core)
    for copy in copies + weight_copies:
        copy.start()
    for copy in copies:
        copy.wait()
    hidden, gain, group, inner, group_prob, expert_prob = targets
    peers, capacity, width = send.shape
    tokens, features = hidden.shape
    groups = slots.shape[0] // capacity
    half = width - LANES
    group_row = group[...]
    strict = (
        lax.broadcasted_iota(jnp.int32, (tokens, tokens), 0)
        < lax.broadcasted_iota(jnp.int32, (tokens, tokens), 1)
    ).astype(BF16)
    slot = lax.broadcasted_iota(jnp.int32, (capacity, tokens), 0)
    one_hot = []
    for g in range(groups):
        member = group_row == g
        flags = jnp.broadcast_to(member.astype(F32), (capacity, tokens)).astype(BF16)
        rank = jnp.dot(flags, strict, preferred_element_type=F32).astype(jnp.int32)
        one_hot.append(((rank == slot) & member).astype(F32))
    picked = jnp.concatenate(one_hot, axis=0).astype(BF16)
    slots[...] = picked
    scaled = expert_prob[...] * group_prob[...]
    expert = lax.broadcasted_iota(jnp.int32, (EPG, tokens), 0)
    weight = jnp.zeros((EPG, tokens), F32)
    for k in range(inner.shape[0]):
        weight += jnp.where(inner[k : k + 1, :] == expert, scaled[k : k + 1, :], 0.0)
    terms = [term.astype(F32) for term in split3(weight)]
    terms.append(jnp.zeros((LANES - 3 * EPG, tokens), F32))
    table = jnp.concatenate(terms, axis=0).astype(BF16)
    rows_weight = lax.dot_general(
        picked, table, (((1,), (1,)), ((), ())), preferred_element_type=F32
    ).astype(BF16)
    wide = hidden[...].astype(F32)
    scale = lax.rsqrt(jnp.sum(wide * wide, axis=-1, keepdims=True) / features + EPS)
    start = pl.multiple_of(core * half, LANES)
    mine = hidden[:, pl.ds(start, half)].astype(F32)
    normed = (mine * scale * gain[:, pl.ds(start, half)]).astype(BF16)
    rows = jnp.dot(picked, normed, preferred_element_type=F32).astype(BF16)
    for p in range(peers):
        g = p * groups // peers
        send[p, :, :half] = rows[g * capacity : (g + 1) * capacity, :]
        send[p, :, half:] = rows_weight[g * capacity : (g + 1) * capacity, :]
    for copy in weight_copies:
        copy.wait()


def first_half_kernel(rows, first, w_gate, w_up, partial, second, sems):
    copies = half_copies((w_gate, w_up), second, sems, 1 - lax.axis_index("tp") % 2)
    for copy in copies:
        copy.start()
    value = rows[:, : first.shape[2]]
    for e in range(first.shape[0]):
        for m in range(2):
            partial[e, m] = jnp.dot(value, first[e, m], preferred_element_type=F32)
    for copy in copies:
        copy.wait()


def second_half_kernel(rows, other, partial, second, w_down, act, down, sem):
    copy = pltpu.make_async_copy(w_down, down, sem)
    copy.start()
    experts, _, half, _ = second.shape
    value = other[:, :half]
    terms = rows[:, half:].astype(F32)
    owners = EPG // experts
    start = (lax.axis_index("ep") % owners) * experts
    lane = lax.broadcasted_iota(jnp.int32, terms.shape, 1)
    for e in range(experts):
        gate = partial[e, 0] + jnp.dot(value, second[e, 0], preferred_element_type=F32)
        up = partial[e, 1] + jnp.dot(value, second[e, 1], preferred_element_type=F32)
        chosen = (lane % EPG == start + e) & (lane < 3 * EPG)
        weight = jnp.sum(jnp.where(chosen, terms, 0.0), axis=-1, keepdims=True)
        act[e] = (gate / (1.0 + jnp.exp(-gate)) * up * weight).astype(BF16)
    copy.wait()


def combine_kernel(returned, slots, out):
    peers, capacity, width = returned.shape
    groups = slots.shape[0] // capacity
    owners = peers // groups
    parts = []
    for g in range(groups):
        parts += [slots[g * capacity : (g + 1) * capacity, :]] * owners
    spread = jnp.concatenate(parts, axis=0)
    value = returned[...].reshape(peers * capacity, width)
    out[...] = lax.dot_general(
        spread, value, (((0,), (0,)), ((), ())), preferred_element_type=F32
    ).astype(BF16)


def down_kernel(act, w_down, sums):
    total = jnp.dot(act[0], w_down[0], preferred_element_type=F32)
    for e in range(1, w_down.shape[0]):
        total += jnp.dot(act[e], w_down[e], preferred_element_type=F32)
    sums[...] = total.astype(BF16)


def kernel_call(body, out_shape, args, stream=(), scratch=(), flops=0, limit=16):
    placed = [pltpu.with_memory_space_constraint(value, pltpu.VMEM) for value in args]
    placed += [pltpu.with_memory_space_constraint(value, pltpu.HBM) for value in stream]
    return pl.pallas_call(
        body,
        out_shape=out_shape,
        in_specs=[pl.BlockSpec(memory_space=pltpu.VMEM)] * len(args) + [ANY] * len(stream),
        scratch_shapes=scratch,
        compiler_params=pltpu.CompilerParams(vmem_limit_bytes=limit * 2**20),
        cost_estimate=pl.CostEstimate(flops=flops, transcendentals=0, bytes_accessed=0),
    )(*placed)


def on_device(
    hidden_in, norm_gain, group_ids, inner_ids, group_prob, expert_prob, w_gate, w_up, w_down
):
    ep_count = lax.axis_size("ep")
    tp_count = lax.axis_size("tp")
    local_count, features, hidden_cols = w_gate.shape
    tokens = hidden_in.shape[0]
    groups = local_count * ep_count // EPG
    capacity = tokens // 2
    rows_count = ep_count * capacity
    half = features // 2
    width = half + LANES
    shape = pltpu.VMEM
    small = (
        hidden_in,
        norm_gain[None, :],
        group_ids[None, :],
        inner_ids.T,
        group_prob[None, :],
        expert_prob.T,
    )
    half_shape = (local_count, 2, half, hidden_cols)
    half_sems = pltpu.SemaphoreType.DMA(half_shape[:2])
    send, slots, first = kernel_call(
        dispatch_kernel,
        (
            shape((ep_count, capacity, width), BF16),
            shape((groups * capacity, tokens), BF16),
            shape(half_shape, BF16),
        ),
        (),
        small + (w_gate, w_up),
        [pltpu.VMEM(value.shape, value.dtype) for value in small]
        + [pltpu.SemaphoreType.DMA((len(small),)), half_sems],
    )
    got = lax.all_to_all(send, "ep", split_axis=0, concat_axis=0, tiled=True)
    rows = got.reshape(rows_count, width)
    swap = [(t, t ^ 1) for t in range(tp_count)]
    other = lax.ppermute(rows, "tp", swap)
    flops = rows_count * half * hidden_cols * local_count * 4
    partial, second = kernel_call(
        first_half_kernel,
        (
            shape((local_count, 2, rows_count, hidden_cols), F32),
            shape(half_shape, BF16),
        ),
        (rows, first),
        (w_gate, w_up),
        [half_sems],
        flops,
    )
    act, w_down = kernel_call(
        second_half_kernel,
        (
            shape((local_count, rows_count, hidden_cols), BF16),
            shape(w_down.shape, BF16),
        ),
        (rows, other, partial, second),
        (w_down,),
        [pltpu.SemaphoreType.DMA],
        flops,
    )
    gathered = lax.all_gather(act, "tp", axis=2, tiled=True)
    out_cols = w_down.shape[2]
    sums = kernel_call(
        down_kernel,
        shape((rows_count, out_cols), BF16),
        (gathered, w_down),
    )
    returned = lax.all_to_all(
        sums.reshape(ep_count, capacity, out_cols),
        "ep",
        split_axis=0,
        concat_axis=0,
        tiled=True,
    )
    return kernel_call(
        combine_kernel,
        jax.ShapeDtypeStruct((tokens, out_cols), BF16),
        (returned, slots),
    )


def solution(mesh):
    placed = (
        P("ep", None),
        P(),
        P("ep"),
        P("ep", None),
        P("ep"),
        P("ep", None),
        P("ep", None, "tp"),
        P("ep", None, "tp"),
        P("ep", None, "tp"),
    )
    return jax.shard_map(
        on_device, mesh=mesh, in_specs=placed, out_specs=P("ep", "tp"), check_vma=False
    )
```

```python
import functools

import jax
import jax.numpy as jnp
from jax import lax
from jax.experimental import pallas as pl
from jax.experimental.pallas import tpu as pltpu
from jax.sharding import PartitionSpec as P

EPG = 8
EPS = 1e-06
LANES = 128
ANY = pl.BlockSpec(memory_space=pl.ANY)
BF16 = jnp.bfloat16
F32 = jnp.float32


def split3(value):
    high = value.astype(BF16)
    rest = value - high.astype(F32)
    mid = rest.astype(BF16)
    low = (rest - mid.astype(F32)).astype(BF16)
    return high, mid, low


def dispatch_kernel(*refs):
    sources, (send, slots), targets, sems = refs[:6], refs[6:8], refs[8:14], refs[14]
    core = lax.axis_index("tp") % 2
    copies = [
        pltpu.make_async_copy(source, target, sems.at[n])
        for n, (source, target) in enumerate(zip(sources, targets))
    ]
    for copy in copies:
        copy.start()
    for copy in copies:
        copy.wait()
    hidden, gain, group, inner, group_prob, expert_prob = targets
    peers, capacity, width = send.shape
    tokens, features = hidden.shape
    groups = slots.shape[0] // capacity
    half = width - LANES
    group_row = group[...]
    strict = (
        lax.broadcasted_iota(jnp.int32, (tokens, tokens), 0)
        < lax.broadcasted_iota(jnp.int32, (tokens, tokens), 1)
    ).astype(BF16)
    slot = lax.broadcasted_iota(jnp.int32, (capacity, tokens), 0)
    one_hot = []
    for g in range(groups):
        member = group_row == g
        flags = jnp.broadcast_to(member.astype(F32), (capacity, tokens)).astype(BF16)
        rank = jnp.dot(flags, strict, preferred_element_type=F32).astype(jnp.int32)
        one_hot.append(((rank == slot) & member).astype(F32))
    picked = jnp.concatenate(one_hot, axis=0).astype(BF16)
    slots[...] = picked
    scaled = expert_prob[...] * group_prob[...]
    expert = lax.broadcasted_iota(jnp.int32, (EPG, tokens), 0)
    weight = jnp.zeros((EPG, tokens), F32)
    for k in range(inner.shape[0]):
        weight += jnp.where(inner[k : k + 1, :] == expert, scaled[k : k + 1, :], 0.0)
    terms = [term.astype(F32) for term in split3(weight)]
    terms.append(jnp.zeros((LANES - 3 * EPG, tokens), F32))
    table = jnp.concatenate(terms, axis=0).astype(BF16)
    rows_weight = lax.dot_general(
        picked, table, (((1,), (1,)), ((), ())), preferred_element_type=F32
    ).astype(BF16)
    wide = hidden[...].astype(F32)
    scale = lax.rsqrt(jnp.sum(wide * wide, axis=-1, keepdims=True) / features + EPS)
    start = pl.multiple_of(core * half, LANES)
    mine = hidden[:, pl.ds(start, half)].astype(F32)
    normed = (mine * scale * gain[:, pl.ds(start, half)]).astype(BF16)
    rows = jnp.dot(picked, normed, preferred_element_type=F32).astype(BF16)
    for p in range(peers):
        g = p * groups // peers
        send[p, :, :half] = rows[g * capacity : (g + 1) * capacity, :]
        send[p, :, half:] = rows_weight[g * capacity : (g + 1) * capacity, :]


def first_half_kernel(rows, w_gate, w_up, partial):
    half = w_gate.shape[1] // 2
    start = pl.multiple_of(lax.axis_index("tp") % 2 * half, LANES)
    value = rows[:, :half]
    for e in range(w_gate.shape[0]):
        for m, source in enumerate((w_gate, w_up)):
            weight = source[e, pl.ds(start, half), :]
            partial[e, m] = jnp.dot(value, weight, preferred_element_type=F32)


def second_half_kernel(rows, other, partial, w_gate, w_up, act):
    experts = w_gate.shape[0]
    half = w_gate.shape[1] // 2
    start = pl.multiple_of((1 - lax.axis_index("tp") % 2) * half, LANES)
    value = other[:, :half]
    terms = rows[:, half:].astype(F32)
    owners = EPG // experts
    first = (lax.axis_index("ep") % owners) * experts
    lane = lax.broadcasted_iota(jnp.int32, terms.shape, 1)
    for e in range(experts):
        gate_weight = w_gate[e, pl.ds(start, half), :]
        up_weight = w_up[e, pl.ds(start, half), :]
        gate = partial[e, 0] + jnp.dot(value, gate_weight, preferred_element_type=F32)
        up = partial[e, 1] + jnp.dot(value, up_weight, preferred_element_type=F32)
        chosen = (lane % EPG == first + e) & (lane < 3 * EPG)
        weight = jnp.sum(jnp.where(chosen, terms, 0.0), axis=-1, keepdims=True)
        act[e] = (gate / (1.0 + jnp.exp(-gate)) * up * weight).astype(BF16)


def combine_kernel(returned, slots, out):
    peers, capacity, width = returned.shape
    groups = slots.shape[0] // capacity
    owners = peers // groups
    parts = []
    for g in range(groups):
        parts += [slots[g * capacity : (g + 1) * capacity, :]] * owners
    spread = jnp.concatenate(parts, axis=0)
    value = returned[...].reshape(peers * capacity, width)
    out[...] = lax.dot_general(
        spread, value, (((0,), (0,)), ((), ())), preferred_element_type=F32
    ).astype(BF16)


def down_kernel(*refs, steps, base):
    acts, w_down, out = refs[: len(steps)], refs[len(steps)], refs[-1]
    tp_count = lax.axis_size("tp")
    me = lax.axis_index("tp")
    cols = acts[0].shape[2]
    total = refs[len(steps) + 1][...] if base else None
    for act, (row, core) in zip(acts, steps):
        owner = (me + tp_count - 2 * row) % tp_count
        owner = owner + core * (1 - 2 * (owner % 2))
        start = pl.multiple_of(owner * cols, LANES)
        for e in range(w_down.shape[0]):
            part = jnp.dot(act[e], w_down[e, pl.ds(start, cols), :], preferred_element_type=F32)
            total = part if total is None else total + part
    out[...] = total.astype(out.dtype)


def kernel_call(body, out_shape, args, stream=(), scratch=(), flops=0, limit=16):
    placed = [pltpu.with_memory_space_constraint(value, pltpu.VMEM) for value in args]
    placed += [pltpu.with_memory_space_constraint(value, pltpu.HBM) for value in stream]
    return pl.pallas_call(
        body,
        out_shape=out_shape,
        in_specs=[pl.BlockSpec(memory_space=pltpu.VMEM)] * len(args) + [ANY] * len(stream),
        scratch_shapes=scratch,
        compiler_params=pltpu.CompilerParams(vmem_limit_bytes=limit * 2**20),
        cost_estimate=pl.CostEstimate(flops=flops, transcendentals=0, bytes_accessed=0),
    )(*placed)


def on_device(
    hidden_in, norm_gain, group_ids, inner_ids, group_prob, expert_prob, w_gate, w_up, w_down
):
    ep_count = lax.axis_size("ep")
    tp_count = lax.axis_size("tp")
    local_count, features, hidden_cols = w_gate.shape
    tokens = hidden_in.shape[0]
    groups = local_count * ep_count // EPG
    capacity = tokens // 2
    rows_count = ep_count * capacity
    half = features // 2
    width = half + LANES
    shape = pltpu.VMEM
    small = (
        hidden_in,
        norm_gain[None, :],
        group_ids[None, :],
        inner_ids.T,
        group_prob[None, :],
        expert_prob.T,
    )
    send, slots = kernel_call(
        dispatch_kernel,
        (
            shape((ep_count, capacity, width), BF16),
            shape((groups * capacity, tokens), BF16),
        ),
        (),
        small,
        [pltpu.VMEM(value.shape, value.dtype) for value in small]
        + [pltpu.SemaphoreType.DMA((len(small),))],
        flops=10**10,
    )
    got = lax.all_to_all(send, "ep", split_axis=0, concat_axis=0, tiled=True)
    rows = got.reshape(rows_count, width)
    swap = [(t, t ^ 1) for t in range(tp_count)]
    other = lax.ppermute(rows, "tp", swap)
    flops = rows_count * half * hidden_cols * local_count * 4
    partial = kernel_call(
        first_half_kernel,
        shape((local_count, 2, rows_count, hidden_cols), F32),
        (rows, w_gate, w_up),
        flops=flops,
    )
    act = kernel_call(
        second_half_kernel,
        shape((local_count, rows_count, hidden_cols), BF16),
        (rows, other, partial, w_gate, w_up),
        flops=flops,
    )
    out_cols = w_down.shape[2]
    rings = [
        [(t, (t + 2 * d) % tp_count) for t in range(tp_count)] for d in range(1, tp_count // 2)
    ]
    far = [lax.ppermute(act, "tp", ring) for ring in rings]
    near = lax.ppermute(act, "tp", swap)
    sums = kernel_call(
        functools.partial(down_kernel, steps=((0, 0), (0, 1)), base=False),
        shape((rows_count, out_cols), F32),
        (act, near, w_down),
        flops=10**8,
    )
    steps = tuple((d + 1, core) for d in range(len(far)) for core in range(2))
    if steps:
        parts = [value for each in far for value in (each, lax.ppermute(each, "tp", swap))]
        sums = kernel_call(
            functools.partial(down_kernel, steps=steps, base=True),
            shape((rows_count, out_cols), BF16),
            (*parts, w_down, sums),
        )
    returned = lax.all_to_all(
        sums.astype(BF16).reshape(ep_count, capacity, out_cols),
        "ep",
        split_axis=0,
        concat_axis=0,
        tiled=True,
    )
    return kernel_call(
        combine_kernel,
        jax.ShapeDtypeStruct((tokens, out_cols), BF16),
        (returned, slots),
    )


def solution(mesh):
    placed = (
        P("ep", None),
        P(),
        P("ep"),
        P("ep", None),
        P("ep"),
        P("ep", None),
        P("ep", None, "tp"),
        P("ep", None, "tp"),
        P("ep", None, "tp"),
    )
    return jax.shard_map(
        on_device, mesh=mesh, in_specs=placed, out_specs=P("ep", "tp"), check_vma=False
    )
```

```python
import functools

import jax
import jax.numpy as jnp
from jax import lax
from jax.experimental import pallas as pl
from jax.experimental.pallas import tpu as pltpu
from jax.sharding import PartitionSpec as P


EPG = 8
EPS = 1e-06
LANES = 128
ANY = pl.BlockSpec(memory_space=pl.ANY)
BF16 = jnp.bfloat16
F32 = jnp.float32


def split3(value):
    high = value.astype(BF16)
    rest = value - high.astype(F32)
    mid = rest.astype(BF16)
    low = (rest - mid.astype(F32)).astype(BF16)
    return high, mid, low


def dispatch_kernel(*refs):
    sources, targets, sems, blocks = refs[:6], refs[-8:-2], refs[-2], refs[-1]
    sends, slots = refs[6:-9], refs[-9]
    capacity, width = sends[0].shape
    groups = len(sends)
    half = width - LANES
    core = lax.axis_index("tp") % 2
    copies = [
        pltpu.make_async_copy(source, target, sems.at[n])
        for n, (source, target) in enumerate(zip(sources, targets))
    ]
    for copy in copies:
        copy.start()
    for copy in copies:
        copy.wait()
    hidden, gain, group, inner, group_prob, expert_prob = targets
    tokens, features = hidden.shape
    group_row = group[...]
    strict = (
        lax.broadcasted_iota(jnp.int32, (tokens, tokens), 0)
        < lax.broadcasted_iota(jnp.int32, (tokens, tokens), 1)
    ).astype(BF16)
    slot = lax.broadcasted_iota(jnp.int32, (capacity, tokens), 0)
    one_hot = []
    for g in range(groups):
        member = group_row == g
        flags = jnp.broadcast_to(member.astype(F32), (capacity, tokens)).astype(BF16)
        rank = jnp.dot(flags, strict, preferred_element_type=F32).astype(jnp.int32)
        one_hot.append(((rank == slot) & member).astype(F32))
    picked = jnp.concatenate(one_hot, axis=0).astype(BF16)
    slots[...] = picked
    scaled = expert_prob[...] * group_prob[...]
    expert = lax.broadcasted_iota(jnp.int32, (EPG, tokens), 0)
    weight = jnp.zeros((EPG, tokens), F32)
    for k in range(inner.shape[0]):
        weight += jnp.where(inner[k : k + 1, :] == expert, scaled[k : k + 1, :], 0.0)
    terms = [term.astype(F32) for term in split3(weight)]
    terms.append(jnp.zeros((LANES - 3 * EPG, tokens), F32))
    table = jnp.concatenate(terms, axis=0).astype(BF16)
    rows_weight = lax.dot_general(
        picked, table, (((1,), (1,)), ((), ())), preferred_element_type=F32
    ).astype(BF16)
    wide = hidden[...].astype(F32)
    scale = lax.rsqrt(jnp.sum(wide * wide, axis=-1, keepdims=True) / features + EPS)
    start = pl.multiple_of(core * half, LANES)
    mine = hidden[:, pl.ds(start, half)].astype(F32)
    normed = (mine * scale * gain[:, pl.ds(start, half)]).astype(BF16)
    rows = jnp.dot(picked, normed, preferred_element_type=F32).astype(BF16)
    for g in range(groups):
        blocks[g, :, :half] = rows[g * capacity : (g + 1) * capacity, :]
        blocks[g, :, half:] = rows_weight[g * capacity : (g + 1) * capacity, :]
    own = lax.axis_index("ep") // (lax.axis_size("ep") // groups)
    for d in range(groups):
        sends[d][...] = blocks[(own + d) % groups]


def pack_kernel(*refs):
    out, row = refs[-1], 0
    for part in refs[:-1]:
        out[row : row + part.shape[0], :] = part[...]
        row += part.shape[0]


def first_half_kernel(rows, w_gate, w_up, partial):
    half = w_gate.shape[1] // 2
    start = pl.multiple_of(lax.axis_index("tp") % 2 * half, LANES)
    value = rows[:, :half]
    for e in range(w_gate.shape[0]):
        for m, source in enumerate((w_gate, w_up)):
            weight = source[e, pl.ds(start, half), :]
            partial[e, m] = jnp.dot(value, weight, preferred_element_type=F32)


def second_half_kernel(rows, other, partial, w_gate, w_up, act):
    experts = w_gate.shape[0]
    half = w_gate.shape[1] // 2
    start = pl.multiple_of((1 - lax.axis_index("tp") % 2) * half, LANES)
    value = other[:, :half]
    terms = rows[:, half:].astype(F32)
    owners = EPG // experts
    first = (lax.axis_index("ep") % owners) * experts
    lane = lax.broadcasted_iota(jnp.int32, terms.shape, 1)
    for e in range(experts):
        gate_weight = w_gate[e, pl.ds(start, half), :]
        up_weight = w_up[e, pl.ds(start, half), :]
        gate = partial[e, 0] + jnp.dot(value, gate_weight, preferred_element_type=F32)
        up = partial[e, 1] + jnp.dot(value, up_weight, preferred_element_type=F32)
        chosen = (lane % EPG == first + e) & (lane < 3 * EPG)
        weight = jnp.sum(jnp.where(chosen, terms, 0.0), axis=-1, keepdims=True)
        act[e] = (gate / (1.0 + jnp.exp(-gate)) * up * weight).astype(BF16)


def combine_kernel(*refs, owners):
    slots, out, parts, returned = refs[-2], refs[-1], refs[:owners], refs[owners:-2]
    groups = 1 + len(returned)
    capacity = slots.shape[0] // groups
    own = lax.axis_index("ep") // owners
    total = parts[0][:capacity, :].astype(F32)
    for part in parts[1:]:
        total += part[:capacity, :].astype(F32)
    values = jnp.concatenate([total.astype(BF16)] + [part[...] for part in returned], axis=0)
    starts = [pl.multiple_of((own + d) % groups * capacity, capacity) for d in range(groups)]
    spread = jnp.concatenate([slots[pl.ds(start, capacity), :] for start in starts], axis=0)
    out[...] = lax.dot_general(
        spread, values, (((0,), (0,)), ((), ())), preferred_element_type=F32
    ).astype(BF16)


def down_sum(acts, w_down, steps, total=None):
    tp_count = lax.axis_size("tp")
    me = lax.axis_index("tp")
    cols = acts[0].shape[2]
    for act, (shift, core) in zip(acts, steps):
        owner = (me + tp_count - 2 * shift) % tp_count
        owner = owner + core * (1 - 2 * (owner % 2))
        start = pl.multiple_of(owner * cols, LANES)
        for e in range(w_down.shape[0]):
            part = jnp.dot(act[e], w_down[e, pl.ds(start, cols), :], preferred_element_type=F32)
            total = part if total is None else total + part
    return total


def down_kernel(*refs, steps):
    acts, w_down, out = refs[: len(steps)], refs[-2], refs[-1]
    out[...] = down_sum(acts, w_down, steps)


def down_last_kernel(*refs, steps, owners):
    acts, w_down, base, outs = refs[: len(steps)], *refs[-owners - 2 : -owners], refs[-owners:]
    total = down_sum(acts, w_down, steps, base[...]).astype(BF16)
    rows = outs[0].shape[0]
    for j, out in enumerate(outs):
        out[...] = total[j * rows : (j + 1) * rows, :]


def owner_sum_kernel(*refs, owners):
    outs, parts = refs[owners:], refs[:owners]
    capacity = outs[0].shape[0]
    total = parts[0][capacity:, :].astype(F32)
    for part in parts[1:]:
        total += part[capacity:, :].astype(F32)
    total = total.astype(BF16)
    for n, out in enumerate(outs):
        out[...] = total[n * capacity : (n + 1) * capacity, :]


def kernel_call(body, out_shape, args, stream=(), scratch=(), flops=0, limit=16):
    placed = [pltpu.with_memory_space_constraint(value, pltpu.VMEM) for value in args]
    placed += [pltpu.with_memory_space_constraint(value, pltpu.HBM) for value in stream]
    return pl.pallas_call(
        body,
        out_shape=out_shape,
        in_specs=[pl.BlockSpec(memory_space=pltpu.VMEM)] * len(args) + [ANY] * len(stream),
        scratch_shapes=scratch,
        compiler_params=pltpu.CompilerParams(vmem_limit_bytes=limit * 2**20),
        cost_estimate=pl.CostEstimate(flops=flops, transcendentals=0, bytes_accessed=0),
    )(*placed)


def on_device(
    hidden_in, norm_gain, group_ids, inner_ids, group_prob, expert_prob, w_gate, w_up, w_down
):
    ep_count = lax.axis_size("ep")
    tp_count = lax.axis_size("tp")
    local_count, features, hidden_cols = w_gate.shape
    tokens = hidden_in.shape[0]
    groups = local_count * ep_count // EPG
    capacity = tokens // 2
    half = features // 2
    width = half + LANES
    shape = pltpu.VMEM
    small = (
        hidden_in,
        norm_gain[None, :],
        group_ids[None, :],
        inner_ids.T,
        group_prob[None, :],
        expert_prob.T,
    )
    owners = EPG // local_count
    *sends, slots = kernel_call(
        dispatch_kernel,
        [shape((capacity, width), BF16)] * groups + [shape((groups * capacity, tokens), BF16)],
        (),
        small,
        [pltpu.VMEM(value.shape, value.dtype) for value in small]
        + [
            pltpu.SemaphoreType.DMA((len(small),)),
            pltpu.VMEM((groups, capacity, width), BF16),
        ],
        flops=10**10,
    )

    def shift_group(value, d):
        pairs = [(s, (s + d * owners) % ep_count) for s in range(ep_count)]
        return lax.ppermute(value, "ep", pairs)

    def to_owner(value, j):
        return lax.ppermute(value, "ep", [(s, s ^ j) for s in range(ep_count)])

    def swap_cores(value):
        return lax.ppermute(value, "tp", [(t, t ^ 1) for t in range(tp_count)])

    def pack(parts):
        if len(parts) == 1:
            return parts[0]
        rows = sum(part.shape[0] for part in parts)
        return kernel_call(pack_kernel, shape((rows, width), BF16), parts)

    far_got = [shift_group(sends[d], d) for d in range(1, groups)]
    far_got = pack(far_got)
    own_parts, far_parts = [sends[0]], [far_got]
    for j in reversed(range(1, owners)):
        own_parts.insert(1, to_owner(sends[0], j))
        far_parts.insert(1, to_owner(far_got, j))
    rows = pack([part for pair in zip(own_parts, far_parts) for part in pair])
    other = swap_cores(rows)
    count = rows.shape[0]
    flops = count * half * hidden_cols * local_count * 4
    partial = kernel_call(
        first_half_kernel,
        shape((local_count, 2, count, hidden_cols), F32),
        (rows, w_gate, w_up),
        flops=flops,
    )
    act = kernel_call(
        second_half_kernel,
        shape((local_count, count, hidden_cols), BF16),
        (rows, other, partial, w_gate, w_up),
        flops=flops,
    )
    far = [
        lax.ppermute(act, "tp", [(t, (t + 2 * d) % tp_count) for t in range(tp_count)])
        for d in range(1, tp_count // 2)
    ]
    near = swap_cores(act)
    far = [value for each in far for value in (each, swap_cores(each))]
    out_cols = w_down.shape[2]
    steps = tuple((d, core) for d in range(tp_count // 2) for core in range(2))
    base = kernel_call(
        functools.partial(down_kernel, steps=steps[:2]),
        shape((count, out_cols), F32),
        (act, near, w_down),
        flops=10**8,
    )
    sums = kernel_call(
        functools.partial(down_last_kernel, steps=steps[2:], owners=owners),
        [shape((count // owners, out_cols), BF16)] * owners,
        (*far, w_down, base),
    )
    gathered = [sums[0]]
    for j in reversed(range(1, owners)):
        gathered.insert(1, to_owner(sums[j], j))
    totals = kernel_call(
        functools.partial(owner_sum_kernel, owners=owners),
        [shape((capacity, out_cols), BF16)] * (groups - 1),
        gathered,
    )
    returned = [shift_group(totals[d - 1], -d) for d in range(1, groups)]
    return kernel_call(
        functools.partial(combine_kernel, owners=owners),
        jax.ShapeDtypeStruct((tokens, out_cols), BF16),
        (*gathered, *returned, slots),
    )


def solution(mesh):
    placed = (
        P("ep", None),
        P(),
        P("ep"),
        P("ep", None),
        P("ep"),
        P("ep", None),
        P("ep", None, "tp"),
        P("ep", None, "tp"),
        P("ep", None, "tp"),
    )

    return jax.shard_map(on_device, mesh=mesh, in_specs=placed, out_specs=P("ep", "tp"), check_vma=False)
```

```python
import functools

import jax
import jax.numpy as jnp
from jax import lax
from jax.experimental import pallas as pl
from jax.experimental.pallas import tpu as pltpu
from jax.sharding import PartitionSpec as P


EPG = 8
EPS = 1e-06
LANES = 128
ANY = pl.BlockSpec(memory_space=pl.ANY)
BF16 = jnp.bfloat16
F32 = jnp.float32


def split3(value):
    high = value.astype(BF16)
    rest = value - high.astype(F32)
    mid = rest.astype(BF16)
    low = (rest - mid.astype(F32)).astype(BF16)
    return high, mid, low


def dispatch_kernel(*refs):
    sources, targets, sems, blocks = refs[:6], refs[-8:-2], refs[-2], refs[-1]
    sends, slots = refs[6:-9], refs[-9]
    capacity, width = sends[0].shape
    groups = len(sends)
    half = width - LANES
    core = lax.axis_index("tp") % 2
    copies = [
        pltpu.make_async_copy(source, target, sems.at[n])
        for n, (source, target) in enumerate(zip(sources, targets))
    ]
    for copy in copies:
        copy.start()
    for copy in copies:
        copy.wait()
    hidden, gain, group, inner, group_prob, expert_prob = targets
    tokens, features = hidden.shape
    group_row = group[...]
    strict = (
        lax.broadcasted_iota(jnp.int32, (tokens, tokens), 0)
        < lax.broadcasted_iota(jnp.int32, (tokens, tokens), 1)
    ).astype(BF16)
    slot = lax.broadcasted_iota(jnp.int32, (capacity, tokens), 0)
    one_hot = []
    for g in range(groups):
        member = group_row == g
        flags = jnp.broadcast_to(member.astype(F32), (capacity, tokens)).astype(BF16)
        rank = jnp.dot(flags, strict, preferred_element_type=F32).astype(jnp.int32)
        one_hot.append(((rank == slot) & member).astype(F32))
    picked = jnp.concatenate(one_hot, axis=0).astype(BF16)
    slots[...] = picked
    scaled = expert_prob[...] * group_prob[...]
    expert = lax.broadcasted_iota(jnp.int32, (EPG, tokens), 0)
    weight = jnp.zeros((EPG, tokens), F32)
    for k in range(inner.shape[0]):
        weight += jnp.where(inner[k : k + 1, :] == expert, scaled[k : k + 1, :], 0.0)
    terms = [term.astype(F32) for term in split3(weight)]
    terms.append(jnp.zeros((LANES - 3 * EPG, tokens), F32))
    table = jnp.concatenate(terms, axis=0).astype(BF16)
    rows_weight = lax.dot_general(
        picked, table, (((1,), (1,)), ((), ())), preferred_element_type=F32
    ).astype(BF16)
    wide = hidden[...].astype(F32)
    scale = lax.rsqrt(jnp.sum(wide * wide, axis=-1, keepdims=True) / features + EPS)
    start = pl.multiple_of(core * half, LANES)
    mine = hidden[:, pl.ds(start, half)].astype(F32)
    normed = (mine * scale * gain[:, pl.ds(start, half)]).astype(BF16)
    rows = jnp.dot(picked, normed, preferred_element_type=F32).astype(BF16)
    for g in range(groups):
        blocks[g, :, :half] = rows[g * capacity : (g + 1) * capacity, :]
        blocks[g, :, half:] = rows_weight[g * capacity : (g + 1) * capacity, :]
    own = lax.axis_index("ep") // (lax.axis_size("ep") // groups)
    for d in range(groups):
        sends[d][...] = blocks[(own + d) % groups]


def pack_kernel(*refs):
    out, row = refs[-1], 0
    for part in refs[:-1]:
        out[row : row + part.shape[0], :] = part[...]
        row += part.shape[0]


def first_half_kernel(rows, w_gate, w_up, partial):
    half = w_gate.shape[1] // 2
    start = pl.multiple_of(lax.axis_index("tp") % 2 * half, LANES)
    value = rows[:, :half]
    for e in range(w_gate.shape[0]):
        for m, source in enumerate((w_gate, w_up)):
            weight = source[e, pl.ds(start, half), :]
            partial[e, m] = jnp.dot(value, weight, preferred_element_type=F32)


def second_half_kernel(rows, near, far, partial, w_gate, w_up, act):
    experts = w_gate.shape[0]
    half = w_gate.shape[1] // 2
    start = pl.multiple_of((1 - lax.axis_index("tp") % 2) * half, LANES)
    value = jnp.concatenate([near[:, :half], far[:, :half]], axis=0)
    terms = rows[:, half:].astype(F32)
    owners = EPG // experts
    first = (lax.axis_index("ep") % owners) * experts
    lane = lax.broadcasted_iota(jnp.int32, terms.shape, 1)
    for e in range(experts):
        gate_weight = w_gate[e, pl.ds(start, half), :]
        up_weight = w_up[e, pl.ds(start, half), :]
        gate = partial[e, 0] + jnp.dot(value, gate_weight, preferred_element_type=F32)
        up = partial[e, 1] + jnp.dot(value, up_weight, preferred_element_type=F32)
        chosen = (lane % EPG == first + e) & (lane < 3 * EPG)
        weight = jnp.sum(jnp.where(chosen, terms, 0.0), axis=-1, keepdims=True)
        act[e] = (gate / (1.0 + jnp.exp(-gate)) * up * weight).astype(BF16)


def combine_kernel(*refs, owners):
    slots, out, parts, returned = refs[-2], refs[-1], refs[:owners], refs[owners:-2]
    groups = 1 + len(returned)
    capacity = slots.shape[0] // groups
    own = lax.axis_index("ep") // owners
    total = parts[0][:capacity, :].astype(F32)
    for part in parts[1:]:
        total += part[:capacity, :].astype(F32)
    values = jnp.concatenate([total.astype(BF16)] + [part[...] for part in returned], axis=0)
    starts = [pl.multiple_of((own + d) % groups * capacity, capacity) for d in range(groups)]
    spread = jnp.concatenate([slots[pl.ds(start, capacity), :] for start in starts], axis=0)
    out[...] = lax.dot_general(
        spread, values, (((0,), (0,)), ((), ())), preferred_element_type=F32
    ).astype(BF16)


def down_sum(acts, w_down, steps, total=None):
    tp_count = lax.axis_size("tp")
    me = lax.axis_index("tp")
    cols = acts[0].shape[2]
    for act, (shift, core) in zip(acts, steps):
        owner = (me + tp_count - 2 * shift) % tp_count
        owner = owner + core * (1 - 2 * (owner % 2))
        start = pl.multiple_of(owner * cols, LANES)
        for e in range(w_down.shape[0]):
            part = jnp.dot(act[e], w_down[e, pl.ds(start, cols), :], preferred_element_type=F32)
            total = part if total is None else total + part
    return total


def down_kernel(*refs, steps):
    acts, w_down, out = refs[: len(steps)], refs[-2], refs[-1]
    out[...] = down_sum(acts, w_down, steps)


def down_last_kernel(*refs, steps, owners, capacity):
    acts, w_down, base, outs = refs[: len(steps)], *refs[-owners - 2 : -owners], refs[-owners:]
    total = down_sum(acts, w_down, steps, base[...]).astype(BF16)
    far = outs[0].shape[0] - capacity
    for j, out in enumerate(outs):
        out[:capacity, :] = total[j * capacity : (j + 1) * capacity, :]
        start = owners * capacity + j * far
        out[capacity:, :] = total[start : start + far, :]


def owner_sum_kernel(*refs, owners):
    outs, parts = refs[owners:], refs[:owners]
    capacity = outs[0].shape[0]
    total = parts[0][capacity:, :].astype(F32)
    for part in parts[1:]:
        total += part[capacity:, :].astype(F32)
    total = total.astype(BF16)
    for n, out in enumerate(outs):
        out[...] = total[n * capacity : (n + 1) * capacity, :]


def kernel_call(body, out_shape, args, stream=(), scratch=(), flops=0, limit=16):
    placed = [pltpu.with_memory_space_constraint(value, pltpu.VMEM) for value in args]
    placed += [pltpu.with_memory_space_constraint(value, pltpu.HBM) for value in stream]
    return pl.pallas_call(
        body,
        out_shape=out_shape,
        in_specs=[pl.BlockSpec(memory_space=pltpu.VMEM)] * len(args) + [ANY] * len(stream),
        scratch_shapes=scratch,
        compiler_params=pltpu.CompilerParams(vmem_limit_bytes=limit * 2**20),
        cost_estimate=pl.CostEstimate(flops=flops, transcendentals=0, bytes_accessed=0),
    )(*placed)


def on_device(
    hidden_in, norm_gain, group_ids, inner_ids, group_prob, expert_prob, w_gate, w_up, w_down
):
    ep_count = lax.axis_size("ep")
    tp_count = lax.axis_size("tp")
    local_count, features, hidden_cols = w_gate.shape
    tokens = hidden_in.shape[0]
    groups = local_count * ep_count // EPG
    capacity = tokens // 2
    half = features // 2
    width = half + LANES
    shape = pltpu.VMEM
    small = (
        hidden_in,
        norm_gain[None, :],
        group_ids[None, :],
        inner_ids.T,
        group_prob[None, :],
        expert_prob.T,
    )
    owners = EPG // local_count
    *sends, slots = kernel_call(
        dispatch_kernel,
        [shape((capacity, width), BF16)] * groups + [shape((groups * capacity, tokens), BF16)],
        (),
        small,
        [pltpu.VMEM(value.shape, value.dtype) for value in small]
        + [
            pltpu.SemaphoreType.DMA((len(small),)),
            pltpu.VMEM((groups, capacity, width), BF16),
        ],
        flops=10**10,
    )

    def shift_group(value, d):
        pairs = [(s, (s + d * owners) % ep_count) for s in range(ep_count)]
        return lax.ppermute(value, "ep", pairs)

    def to_owner(value, j):
        return lax.ppermute(value, "ep", [(s, s ^ j) for s in range(ep_count)])

    def swap_cores(value):
        return lax.ppermute(value, "tp", [(t, t ^ 1) for t in range(tp_count)])

    def pack(parts):
        if len(parts) == 1:
            return parts[0]
        rows = sum(part.shape[0] for part in parts)
        return kernel_call(pack_kernel, shape((rows, width), BF16), parts)

    far_got = [shift_group(sends[d], d) for d in range(1, groups)]
    far_got = pack(far_got)
    own_parts, far_parts = [sends[0]], [far_got]
    for j in reversed(range(1, owners)):
        own_parts.insert(1, to_owner(sends[0], j))
        far_parts.insert(1, to_owner(far_got, j))
    near_rows = pack(own_parts)
    near_other = swap_cores(near_rows)
    far_rows = pack(far_parts)
    far_other = swap_cores(far_rows)
    rows = pack([near_rows, far_rows])
    count = rows.shape[0]
    flops = count * half * hidden_cols * local_count * 4
    partial = kernel_call(
        first_half_kernel,
        shape((local_count, 2, count, hidden_cols), F32),
        (rows, w_gate, w_up),
        flops=flops,
    )
    act = kernel_call(
        second_half_kernel,
        shape((local_count, count, hidden_cols), BF16),
        (rows, near_other, far_other, partial, w_gate, w_up),
        flops=flops,
    )
    far = [
        lax.ppermute(act, "tp", [(t, (t + 2 * d) % tp_count) for t in range(tp_count)])
        for d in range(1, tp_count // 2)
    ]
    near = swap_cores(act)
    far = [value for each in far for value in (each, swap_cores(each))]
    out_cols = w_down.shape[2]
    steps = tuple((d, core) for d in range(tp_count // 2) for core in range(2))
    base = kernel_call(
        functools.partial(down_kernel, steps=steps[:2]),
        shape((count, out_cols), F32),
        (act, near, w_down),
        flops=10**8,
    )
    sums = kernel_call(
        functools.partial(
            down_last_kernel, steps=steps[2:], owners=owners, capacity=capacity
        ),
        [shape((count // owners, out_cols), BF16)] * owners,
        (*far, w_down, base),
    )
    gathered = [sums[0]]
    for j in reversed(range(1, owners)):
        gathered.insert(1, to_owner(sums[j], j))
    totals = kernel_call(
        functools.partial(owner_sum_kernel, owners=owners),
        [shape((capacity, out_cols), BF16)] * (groups - 1),
        gathered,
    )
    returned = [shift_group(totals[d - 1], -d) for d in range(1, groups)]
    return kernel_call(
        functools.partial(combine_kernel, owners=owners),
        jax.ShapeDtypeStruct((tokens, out_cols), BF16),
        (*gathered, *returned, slots),
    )


def solution(mesh):
    placed = (
        P("ep", None),
        P(),
        P("ep"),
        P("ep", None),
        P("ep"),
        P("ep", None),
        P("ep", None, "tp"),
        P("ep", None, "tp"),
        P("ep", None, "tp"),
    )

    return jax.shard_map(on_device, mesh=mesh, in_specs=placed, out_specs=P("ep", "tp"), check_vma=False)
```

```python
import functools

import jax
import jax.numpy as jnp
from jax import lax
from jax.experimental import pallas as pl
from jax.experimental.pallas import tpu as pltpu
from jax.sharding import PartitionSpec as P


EPG = 8
EPS = 1e-06
LANES = 128
ANY = pl.BlockSpec(memory_space=pl.ANY)
BF16 = jnp.bfloat16
F32 = jnp.float32


def split3(value):
    high = value.astype(BF16)
    rest = value - high.astype(F32)
    mid = rest.astype(BF16)
    low = (rest - mid.astype(F32)).astype(BF16)
    return high, mid, low


def dispatch_kernel(*refs):
    sources, targets, sems, blocks = refs[:6], refs[-8:-2], refs[-2], refs[-1]
    sends, slots = refs[6:-9], refs[-9]
    capacity, width = sends[0].shape
    groups = len(sends)
    half = width - LANES
    core = lax.axis_index("tp") % 2
    copies = [
        pltpu.make_async_copy(source, target, sems.at[n])
        for n, (source, target) in enumerate(zip(sources, targets))
    ]
    for copy in copies:
        copy.start()
    for copy in copies:
        copy.wait()
    hidden, gain, group, inner, group_prob, expert_prob = targets
    tokens, features = hidden.shape
    group_row = group[...]
    strict = (
        lax.broadcasted_iota(jnp.int32, (tokens, tokens), 0)
        < lax.broadcasted_iota(jnp.int32, (tokens, tokens), 1)
    ).astype(BF16)
    slot = lax.broadcasted_iota(jnp.int32, (capacity, tokens), 0)
    one_hot = []
    for g in range(groups):
        member = group_row == g
        flags = jnp.broadcast_to(member.astype(F32), (capacity, tokens)).astype(BF16)
        rank = jnp.dot(flags, strict, preferred_element_type=F32).astype(jnp.int32)
        one_hot.append(((rank == slot) & member).astype(F32))
    picked = jnp.concatenate(one_hot, axis=0).astype(BF16)
    slots[...] = picked
    scaled = expert_prob[...] * group_prob[...]
    expert = lax.broadcasted_iota(jnp.int32, (EPG, tokens), 0)
    weight = jnp.zeros((EPG, tokens), F32)
    for k in range(inner.shape[0]):
        weight += jnp.where(inner[k : k + 1, :] == expert, scaled[k : k + 1, :], 0.0)
    terms = [term.astype(F32) for term in split3(weight)]
    terms.append(jnp.zeros((LANES - 3 * EPG, tokens), F32))
    table = jnp.concatenate(terms, axis=0).astype(BF16)
    rows_weight = lax.dot_general(
        picked, table, (((1,), (1,)), ((), ())), preferred_element_type=F32
    ).astype(BF16)
    wide = hidden[...].astype(F32)
    scale = lax.rsqrt(jnp.sum(wide * wide, axis=-1, keepdims=True) / features + EPS)
    start = pl.multiple_of(core * half, LANES)
    mine = hidden[:, pl.ds(start, half)].astype(F32)
    normed = (mine * scale * gain[:, pl.ds(start, half)]).astype(BF16)
    rows = jnp.dot(picked, normed, preferred_element_type=F32).astype(BF16)
    for g in range(groups):
        blocks[g, :, :half] = rows[g * capacity : (g + 1) * capacity, :]
        blocks[g, :, half:] = rows_weight[g * capacity : (g + 1) * capacity, :]
    own = lax.axis_index("ep") // (lax.axis_size("ep") // groups)
    for d in range(groups):
        sends[d][...] = blocks[(own + d) % groups]


def pack_kernel(*refs):
    out, row = refs[-1], 0
    for part in refs[:-1]:
        out[row : row + part.shape[0], :] = part[...]
        row += part.shape[0]


def first_half_kernel(rows, w_gate, w_up, partial):
    half = w_gate.shape[1] // 2
    start = pl.multiple_of(lax.axis_index("tp") % 2 * half, LANES)
    value = rows[:, :half]
    for e in range(w_gate.shape[0]):
        for m, source in enumerate((w_gate, w_up)):
            weight = source[e, pl.ds(start, half), :]
            partial[e, m] = jnp.dot(value, weight, preferred_element_type=F32)


def second_half_kernel(rows, near, far, partial, w_gate, w_up, act):
    experts = w_gate.shape[0]
    half = w_gate.shape[1] // 2
    start = pl.multiple_of((1 - lax.axis_index("tp") % 2) * half, LANES)
    value = jnp.concatenate([near[:, :half], far[:, :half]], axis=0)
    terms = rows[:, half:].astype(F32)
    owners = EPG // experts
    first = (lax.axis_index("ep") % owners) * experts
    lane = lax.broadcasted_iota(jnp.int32, terms.shape, 1)
    for e in range(experts):
        gate_weight = w_gate[e, pl.ds(start, half), :]
        up_weight = w_up[e, pl.ds(start, half), :]
        gate = partial[e, 0] + jnp.dot(value, gate_weight, preferred_element_type=F32)
        up = partial[e, 1] + jnp.dot(value, up_weight, preferred_element_type=F32)
        chosen = (lane % EPG == first + e) & (lane < 3 * EPG)
        weight = jnp.sum(jnp.where(chosen, terms, 0.0), axis=-1, keepdims=True)
        act[e] = (gate / (1.0 + jnp.exp(-gate)) * up * weight).astype(BF16)


def combine_kernel(*refs, owners):
    slots, out, parts, returned = refs[-2], refs[-1], refs[:owners], refs[owners:-2]
    groups = 1 + len(returned)
    capacity = slots.shape[0] // groups
    own = lax.axis_index("ep") // owners
    total = parts[0][:capacity, :].astype(F32)
    for part in parts[1:]:
        total += part[:capacity, :].astype(F32)
    values = jnp.concatenate([total.astype(BF16)] + [part[...] for part in returned], axis=0)
    starts = [pl.multiple_of((own + d) % groups * capacity, capacity) for d in range(groups)]
    spread = jnp.concatenate([slots[pl.ds(start, capacity), :] for start in starts], axis=0)
    out[...] = lax.dot_general(
        spread, values, (((0,), (0,)), ((), ())), preferred_element_type=F32
    ).astype(BF16)


def down_sum(acts, w_down, steps, total=None):
    tp_count = lax.axis_size("tp")
    me = lax.axis_index("tp")
    cols = acts[0].shape[2]
    for act, (shift, core) in zip(acts, steps):
        owner = (me + tp_count - 2 * shift) % tp_count
        owner = owner + core * (1 - 2 * (owner % 2))
        start = pl.multiple_of(owner * cols, LANES)
        for e in range(w_down.shape[0]):
            part = jnp.dot(act[e], w_down[e, pl.ds(start, cols), :], preferred_element_type=F32)
            total = part if total is None else total + part
    return total


def down_kernel(*refs, steps, base=False):
    acts, w_down, out = refs[: len(steps)], refs[len(steps)], refs[-1]
    out[...] = down_sum(acts, w_down, steps, refs[-2][...] if base else None)


def down_last_kernel(*refs, steps, owners, capacity):
    acts, w_down, base, outs = refs[: len(steps)], *refs[-owners - 2 : -owners], refs[-owners:]
    total = down_sum(acts, w_down, steps, base[...]).astype(BF16)
    far = outs[0].shape[0] - capacity
    for j, out in enumerate(outs):
        out[:capacity, :] = total[j * capacity : (j + 1) * capacity, :]
        start = owners * capacity + j * far
        out[capacity:, :] = total[start : start + far, :]


def owner_sum_kernel(*refs, owners):
    outs, parts = refs[owners:], refs[:owners]
    capacity = outs[0].shape[0]
    total = parts[0][capacity:, :].astype(F32)
    for part in parts[1:]:
        total += part[capacity:, :].astype(F32)
    total = total.astype(BF16)
    for n, out in enumerate(outs):
        out[...] = total[n * capacity : (n + 1) * capacity, :]


def kernel_call(body, out_shape, args, stream=(), scratch=(), flops=0, limit=16):
    placed = [pltpu.with_memory_space_constraint(value, pltpu.VMEM) for value in args]
    placed += [pltpu.with_memory_space_constraint(value, pltpu.HBM) for value in stream]
    return pl.pallas_call(
        body,
        out_shape=out_shape,
        in_specs=[pl.BlockSpec(memory_space=pltpu.VMEM)] * len(args) + [ANY] * len(stream),
        scratch_shapes=scratch,
        compiler_params=pltpu.CompilerParams(vmem_limit_bytes=limit * 2**20),
        cost_estimate=pl.CostEstimate(flops=flops, transcendentals=0, bytes_accessed=0),
    )(*placed)


def on_device(
    hidden_in, norm_gain, group_ids, inner_ids, group_prob, expert_prob, w_gate, w_up, w_down
):
    ep_count = lax.axis_size("ep")
    tp_count = lax.axis_size("tp")
    local_count, features, hidden_cols = w_gate.shape
    tokens = hidden_in.shape[0]
    groups = local_count * ep_count // EPG
    capacity = tokens // 2
    half = features // 2
    width = half + LANES
    shape = pltpu.VMEM
    small = (
        hidden_in,
        norm_gain[None, :],
        group_ids[None, :],
        inner_ids.T,
        group_prob[None, :],
        expert_prob.T,
    )
    owners = EPG // local_count
    *sends, slots = kernel_call(
        dispatch_kernel,
        [shape((capacity, width), BF16)] * groups + [shape((groups * capacity, tokens), BF16)],
        (),
        small,
        [pltpu.VMEM(value.shape, value.dtype) for value in small]
        + [
            pltpu.SemaphoreType.DMA((len(small),)),
            pltpu.VMEM((groups, capacity, width), BF16),
        ],
        flops=10**10,
    )

    def shift_group(value, d):
        pairs = [(s, (s + d * owners) % ep_count) for s in range(ep_count)]
        return lax.ppermute(value, "ep", pairs)

    def to_owner(value, j):
        return lax.ppermute(value, "ep", [(s, s ^ j) for s in range(ep_count)])

    def swap_cores(value):
        return lax.ppermute(value, "tp", [(t, t ^ 1) for t in range(tp_count)])

    def pack(parts):
        if len(parts) == 1:
            return parts[0]
        rows = sum(part.shape[0] for part in parts)
        return kernel_call(pack_kernel, shape((rows, width), BF16), parts)

    far_got = [shift_group(sends[d], d) for d in range(1, groups)]
    far_got = pack(far_got)
    own_parts, far_parts = [sends[0]], [far_got]
    for j in reversed(range(1, owners)):
        own_parts.insert(1, to_owner(sends[0], j))
        far_parts.insert(1, to_owner(far_got, j))
    near_rows = pack(own_parts)
    near_other = swap_cores(near_rows)
    far_rows = pack(far_parts)
    far_other = swap_cores(far_rows)
    rows = pack([near_rows, far_rows])
    count = rows.shape[0]
    flops = count * half * hidden_cols * local_count * 4
    partial = kernel_call(
        first_half_kernel,
        shape((local_count, 2, count, hidden_cols), F32),
        (rows, w_gate, w_up),
        flops=flops,
    )
    act = kernel_call(
        second_half_kernel,
        shape((local_count, count, hidden_cols), BF16),
        (rows, near_other, far_other, partial, w_gate, w_up),
        flops=flops,
    )
    far = [
        lax.ppermute(act, "tp", [(t, (t + 2 * d) % tp_count) for t in range(tp_count)])
        for d in range(1, tp_count // 2)
    ]
    near = swap_cores(act)
    far = [value for each in far for value in (each, swap_cores(each))]
    out_cols = w_down.shape[2]
    steps = tuple((d, core) for d in range(tp_count // 2) for core in range(2))
    base = kernel_call(
        functools.partial(down_kernel, steps=steps[:2]),
        shape((count, out_cols), F32),
        (act, near, w_down),
        flops=10**8,
    )
    direct = tuple(step for step in steps[2:] if not step[1])
    swapped = tuple(step for step in steps[2:] if step[1])
    base = kernel_call(
        functools.partial(down_kernel, steps=direct, base=True),
        shape((count, out_cols), F32),
        (*far[::2], w_down, base),
        flops=10**8,
    )
    sums = kernel_call(
        functools.partial(
            down_last_kernel, steps=swapped, owners=owners, capacity=capacity
        ),
        [shape((count // owners, out_cols), BF16)] * owners,
        (*far[1::2], w_down, base),
    )
    gathered = [sums[0]]
    for j in reversed(range(1, owners)):
        gathered.insert(1, to_owner(sums[j], j))
    totals = kernel_call(
        functools.partial(owner_sum_kernel, owners=owners),
        [shape((capacity, out_cols), BF16)] * (groups - 1),
        gathered,
    )
    returned = [shift_group(totals[d - 1], -d) for d in range(1, groups)]
    return kernel_call(
        functools.partial(combine_kernel, owners=owners),
        jax.ShapeDtypeStruct((tokens, out_cols), BF16),
        (*gathered, *returned, slots),
    )


def solution(mesh):
    placed = (
        P("ep", None),
        P(),
        P("ep"),
        P("ep", None),
        P("ep"),
        P("ep", None),
        P("ep", None, "tp"),
        P("ep", None, "tp"),
        P("ep", None, "tp"),
    )

    return jax.shard_map(on_device, mesh=mesh, in_specs=placed, out_specs=P("ep", "tp"), check_vma=False)
```

```python
import functools

import jax
import jax.numpy as jnp
from jax import lax
from jax.experimental import pallas as pl
from jax.experimental.pallas import tpu as pltpu
from jax.sharding import PartitionSpec as P


EPG = 8
EPS = 1e-06
LANES = 128
ANY = pl.BlockSpec(memory_space=pl.ANY)
BF16 = jnp.bfloat16
F32 = jnp.float32


def split3(value):
    high = value.astype(BF16)
    rest = value - high.astype(F32)
    mid = rest.astype(BF16)
    low = (rest - mid.astype(F32)).astype(BF16)
    return high, mid, low


def dispatch_kernel(*refs):
    sources, targets, sems, blocks = refs[:6], refs[-8:-2], refs[-2], refs[-1]
    sends, slots = refs[6:-9], refs[-9]
    capacity, width = sends[0].shape
    groups = len(sends)
    half = width - LANES
    core = lax.axis_index("tp") % 2
    copies = [
        pltpu.make_async_copy(source, target, sems.at[n])
        for n, (source, target) in enumerate(zip(sources, targets))
    ]
    for copy in copies:
        copy.start()
    for copy in copies:
        copy.wait()
    hidden, gain, group, inner, group_prob, expert_prob = targets
    tokens, features = hidden.shape
    group_row = group[...]
    strict = (
        lax.broadcasted_iota(jnp.int32, (tokens, tokens), 0)
        < lax.broadcasted_iota(jnp.int32, (tokens, tokens), 1)
    ).astype(BF16)
    slot = lax.broadcasted_iota(jnp.int32, (capacity, tokens), 0)
    one_hot = []
    for g in range(groups):
        member = group_row == g
        flags = jnp.broadcast_to(member.astype(F32), (capacity, tokens)).astype(BF16)
        rank = jnp.dot(flags, strict, preferred_element_type=F32).astype(jnp.int32)
        one_hot.append(((rank == slot) & member).astype(F32))
    picked = jnp.concatenate(one_hot, axis=0).astype(BF16)
    slots[...] = picked
    scaled = expert_prob[...] * group_prob[...]
    expert = lax.broadcasted_iota(jnp.int32, (EPG, tokens), 0)
    weight = jnp.zeros((EPG, tokens), F32)
    for k in range(inner.shape[0]):
        weight += jnp.where(inner[k : k + 1, :] == expert, scaled[k : k + 1, :], 0.0)
    terms = [term.astype(F32) for term in split3(weight)]
    terms.append(jnp.zeros((LANES - 3 * EPG, tokens), F32))
    table = jnp.concatenate(terms, axis=0).astype(BF16)
    rows_weight = lax.dot_general(
        picked, table, (((1,), (1,)), ((), ())), preferred_element_type=F32
    ).astype(BF16)
    wide = hidden[...].astype(F32)
    scale = lax.rsqrt(jnp.sum(wide * wide, axis=-1, keepdims=True) / features + EPS)
    start = pl.multiple_of(core * half, LANES)
    mine = hidden[:, pl.ds(start, half)].astype(F32)
    normed = (mine * scale * gain[:, pl.ds(start, half)]).astype(BF16)
    rows = jnp.dot(picked, normed, preferred_element_type=F32).astype(BF16)
    for g in range(groups):
        blocks[g, :, :half] = rows[g * capacity : (g + 1) * capacity, :]
        blocks[g, :, half:] = rows_weight[g * capacity : (g + 1) * capacity, :]
    own = lax.axis_index("ep") // (lax.axis_size("ep") // groups)
    for d in range(groups):
        sends[d][...] = blocks[(own + d) % groups]


def pack_kernel(*refs):
    out, row = refs[-1], 0
    for part in refs[:-1]:
        out[row : row + part.shape[0], :] = part[...]
        row += part.shape[0]


def first_half_kernel(rows, w_gate, w_up, partial):
    half = w_gate.shape[1] // 2
    start = pl.multiple_of(lax.axis_index("tp") % 2 * half, LANES)
    value = rows[:, :half]
    for e in range(w_gate.shape[0]):
        for m, source in enumerate((w_gate, w_up)):
            weight = source[e, pl.ds(start, half), :]
            partial[e, m] = jnp.dot(value, weight, preferred_element_type=F32)


def second_half_kernel(rows, near, far, partial, w_gate, w_up, act):
    experts = w_gate.shape[0]
    half = w_gate.shape[1] // 2
    start = pl.multiple_of((1 - lax.axis_index("tp") % 2) * half, LANES)
    value = jnp.concatenate([near[:, :half], far[:, :half]], axis=0)
    terms = rows[:, half:].astype(F32)
    owners = EPG // experts
    first = (lax.axis_index("ep") % owners) * experts
    lane = lax.broadcasted_iota(jnp.int32, terms.shape, 1)
    for e in range(experts):
        gate_weight = w_gate[e, pl.ds(start, half), :]
        up_weight = w_up[e, pl.ds(start, half), :]
        gate = partial[e, 0] + jnp.dot(value, gate_weight, preferred_element_type=F32)
        up = partial[e, 1] + jnp.dot(value, up_weight, preferred_element_type=F32)
        chosen = (lane % EPG == first + e) & (lane < 3 * EPG)
        weight = jnp.sum(jnp.where(chosen, terms, 0.0), axis=-1, keepdims=True)
        act[e] = (gate / (1.0 + jnp.exp(-gate)) * up * weight).astype(BF16)


def spread_rows(slots, values, shifts, groups, owners):
    capacity = slots.shape[0] // groups
    own = lax.axis_index("ep") // owners
    starts = [pl.multiple_of((own + d) % groups * capacity, capacity) for d in shifts]
    spread = jnp.concatenate([slots[pl.ds(start, capacity), :] for start in starts], axis=0)
    return lax.dot_general(spread, values, (((0,), (0,)), ((), ())), preferred_element_type=F32)


def place_kernel(*refs, owners, groups):
    slots, out, parts = refs[-2], refs[-1], refs[:owners]
    capacity = slots.shape[0] // groups
    total = parts[0][:capacity, :].astype(F32)
    for part in parts[1:]:
        total += part[:capacity, :].astype(F32)
    out[...] = spread_rows(slots, total.astype(BF16), (0,), groups, owners)


def combine_kernel(*refs, owners, groups):
    returned, placed, slots, out = refs[:-3], refs[-3], refs[-2], refs[-1]
    values = jnp.concatenate([part[...] for part in returned], axis=0)
    rows = spread_rows(slots, values, tuple(range(1, groups)), groups, owners)
    out[...] = (placed[...] + rows).astype(BF16)


def down_sum(acts, w_down, steps, total=None):
    tp_count = lax.axis_size("tp")
    me = lax.axis_index("tp")
    cols = acts[0].shape[2]
    for act, (shift, core) in zip(acts, steps):
        owner = (me + tp_count - 2 * shift) % tp_count
        owner = owner + core * (1 - 2 * (owner % 2))
        start = pl.multiple_of(owner * cols, LANES)
        for e in range(w_down.shape[0]):
            part = jnp.dot(act[e], w_down[e, pl.ds(start, cols), :], preferred_element_type=F32)
            total = part if total is None else total + part
    return total


def down_kernel(*refs, steps, base=False):
    acts, w_down, out = refs[: len(steps)], refs[len(steps)], refs[-1]
    out[...] = down_sum(acts, w_down, steps, refs[-2][...] if base else None)


def down_last_kernel(*refs, steps, owners, capacity):
    acts, w_down, base, outs = refs[: len(steps)], *refs[-owners - 2 : -owners], refs[-owners:]
    total = down_sum(acts, w_down, steps, base[...]).astype(BF16)
    far = outs[0].shape[0] - capacity
    for j, out in enumerate(outs):
        out[:capacity, :] = total[j * capacity : (j + 1) * capacity, :]
        start = owners * capacity + j * far
        out[capacity:, :] = total[start : start + far, :]


def owner_sum_kernel(*refs, owners):
    outs, parts = refs[owners:], refs[:owners]
    capacity = outs[0].shape[0]
    total = parts[0][capacity:, :].astype(F32)
    for part in parts[1:]:
        total += part[capacity:, :].astype(F32)
    total = total.astype(BF16)
    for n, out in enumerate(outs):
        out[...] = total[n * capacity : (n + 1) * capacity, :]


def kernel_call(body, out_shape, args, stream=(), scratch=(), flops=0, limit=16):
    placed = [pltpu.with_memory_space_constraint(value, pltpu.VMEM) for value in args]
    placed += [pltpu.with_memory_space_constraint(value, pltpu.HBM) for value in stream]
    return pl.pallas_call(
        body,
        out_shape=out_shape,
        in_specs=[pl.BlockSpec(memory_space=pltpu.VMEM)] * len(args) + [ANY] * len(stream),
        scratch_shapes=scratch,
        compiler_params=pltpu.CompilerParams(vmem_limit_bytes=limit * 2**20),
        cost_estimate=pl.CostEstimate(flops=flops, transcendentals=0, bytes_accessed=0),
    )(*placed)


def on_device(
    hidden_in, norm_gain, group_ids, inner_ids, group_prob, expert_prob, w_gate, w_up, w_down
):
    ep_count = lax.axis_size("ep")
    tp_count = lax.axis_size("tp")
    local_count, features, hidden_cols = w_gate.shape
    tokens = hidden_in.shape[0]
    groups = local_count * ep_count // EPG
    capacity = tokens // 2
    half = features // 2
    width = half + LANES
    shape = pltpu.VMEM
    small = (
        hidden_in,
        norm_gain[None, :],
        group_ids[None, :],
        inner_ids.T,
        group_prob[None, :],
        expert_prob.T,
    )
    owners = EPG // local_count
    *sends, slots = kernel_call(
        dispatch_kernel,
        [shape((capacity, width), BF16)] * groups + [shape((groups * capacity, tokens), BF16)],
        (),
        small,
        [pltpu.VMEM(value.shape, value.dtype) for value in small]
        + [
            pltpu.SemaphoreType.DMA((len(small),)),
            pltpu.VMEM((groups, capacity, width), BF16),
        ],
        flops=10**10,
    )

    def shift_group(value, d):
        pairs = [(s, (s + d * owners) % ep_count) for s in range(ep_count)]
        return lax.ppermute(value, "ep", pairs)

    def to_owner(value, j):
        return lax.ppermute(value, "ep", [(s, s ^ j) for s in range(ep_count)])

    def swap_cores(value):
        return lax.ppermute(value, "tp", [(t, t ^ 1) for t in range(tp_count)])

    def pack(parts):
        if len(parts) == 1:
            return parts[0]
        rows = sum(part.shape[0] for part in parts)
        return kernel_call(pack_kernel, shape((rows, width), BF16), parts)

    far_got = [shift_group(sends[d], d) for d in range(1, groups)]
    far_got = pack(far_got)
    own_parts, far_parts = [sends[0]], [far_got]
    for j in reversed(range(1, owners)):
        own_parts.insert(1, to_owner(sends[0], j))
        far_parts.insert(1, to_owner(far_got, j))
    near_rows = pack(own_parts)
    near_other = swap_cores(near_rows)
    far_rows = pack(far_parts)
    far_other = swap_cores(far_rows)
    rows = pack([near_rows, far_rows])
    count = rows.shape[0]
    flops = count * half * hidden_cols * local_count * 4
    partial = kernel_call(
        first_half_kernel,
        shape((local_count, 2, count, hidden_cols), F32),
        (rows, w_gate, w_up),
        flops=flops,
    )
    act = kernel_call(
        second_half_kernel,
        shape((local_count, count, hidden_cols), BF16),
        (rows, near_other, far_other, partial, w_gate, w_up),
        flops=flops,
    )
    far = [
        lax.ppermute(act, "tp", [(t, (t + 2 * d) % tp_count) for t in range(tp_count)])
        for d in range(1, tp_count // 2)
    ]
    near = swap_cores(act)
    far = [value for each in far for value in (each, swap_cores(each))]
    out_cols = w_down.shape[2]
    steps = tuple((d, core) for d in range(tp_count // 2) for core in range(2))
    base = kernel_call(
        functools.partial(down_kernel, steps=steps[:2]),
        shape((count, out_cols), F32),
        (act, near, w_down),
        flops=10**8,
    )
    direct = tuple(step for step in steps[2:] if not step[1])
    swapped = tuple(step for step in steps[2:] if step[1])
    base = kernel_call(
        functools.partial(down_kernel, steps=direct, base=True),
        shape((count, out_cols), F32),
        (*far[::2], w_down, base),
        flops=10**8,
    )
    sums = kernel_call(
        functools.partial(
            down_last_kernel, steps=swapped, owners=owners, capacity=capacity
        ),
        [shape((count // owners, out_cols), BF16)] * owners,
        (*far[1::2], w_down, base),
    )
    gathered = [sums[0]]
    for j in reversed(range(1, owners)):
        gathered.insert(1, to_owner(sums[j], j))
    totals = kernel_call(
        functools.partial(owner_sum_kernel, owners=owners),
        [shape((capacity, out_cols), BF16)] * (groups - 1),
        gathered,
    )
    returned = [shift_group(totals[d - 1], -d) for d in range(1, groups)]
    placed = kernel_call(
        functools.partial(place_kernel, owners=owners, groups=groups),
        shape((tokens, out_cols), F32),
        (*gathered, slots),
        flops=10**8,
    )
    return kernel_call(
        functools.partial(combine_kernel, owners=owners, groups=groups),
        jax.ShapeDtypeStruct((tokens, out_cols), BF16),
        (*returned, placed, slots),
    )


def solution(mesh):
    placed = (
        P("ep", None),
        P(),
        P("ep"),
        P("ep", None),
        P("ep"),
        P("ep", None),
        P("ep", None, "tp"),
        P("ep", None, "tp"),
        P("ep", None, "tp"),
    )

    return jax.shard_map(on_device, mesh=mesh, in_specs=placed, out_specs=P("ep", "tp"), check_vma=False)
```
